32 devices in a mesh: fs: 16 (over z, y, x), tp: 2 (over core).
Axes of the slice: x: 2, y: 2, z: 4, core: 2. Of those that a mesh axis runs over, the one named last changes fastest.
Arguments:
- tokens: bfloat16 [2048, 2048], P('fs', 'tp'), may hold values from -300 to 300
- norm_gain: float32 [2048], P('fs'), may hold values from 0.1 to 1.9
- gate_weight: float32 [16, 2048, 1024], P(None, 'fs', 'tp'), may hold values from -1.3258252 to 1.3258252
- up_weight: float32 [16, 2048, 1024], P(None, 'fs', 'tp'), may hold values from -1.3258252 to 1.3258252
- down_weight: float32 [16, 1024, 2048], P(None, 'fs', 'tp'), may hold values from -0.1875 to 0.1875
- routes: int32 [2048, 4], P('fs'), may hold values from 0 to 15, all different within a row; in each aligned block of 128 rows (0 to 127, 128 to 255, ...) at most 64 rows name the same one
- route_weights: float32 [2048, 4], P('fs'), may hold values from 0.05 to 1
Outputs:
- mixed: bfloat16 [2048, 2048], P('fs', 'tp')
- gate_ready: bfloat16 [16, 2048, 1024], P('fs', None, 'tp')
- up_ready: bfloat16 [16, 2048, 1024], P('fs', None, 'tp')
- down_ready: bfloat16 [16, 1024, 2048], P('fs', None, 'tp')
The draws below stay inside these ranges and needn't reach their ends.
Inputs may be any that keep to these rules, and one draw needn't show every extreme that they name: `routes`: each row names 4 different experts. In each aligned block of 128 rows no expert is named more than 64 times, a bound that some block reaches.
All inputs are finite; a program needn't handle non-finite values.
Results may differ from the reference program's by a relative error of at most 0.0089.
Values may be sent and summed in bfloat16 or wider, within the bound.
No kernel may reach another device: no remote copies, remote signals or barrier semaphores. Data moves between devices by JAX's collectives and lax.ppermute only.
A program may use at most 64 MiB of HBM per device.

```python
import math
import jax
import jax.numpy as jnp
import numpy as np
from jax import lax

D = 2048
FF = 1024
TOP_K = 4
TOK_DEV = 128
EXPERTS = 16
CAP = 64
TOKENS = 2048
N_FS = 16


def expert_matrix(key, salt):
    base = jax.random.fold_in(key, salt)
    noise = jax.random.truncated_normal(jax.random.fold_in(base, 1), -6.0, 6.0, (EXPERTS, D, FF), jnp.float32)
    column = jnp.exp(jax.random.uniform(jax.random.fold_in(base, 2), (EXPERTS, 1, FF), jnp.float32, math.log(0.5), math.log(3.0)))
    return noise * column * D ** (-0.5)


def draw_gate_weight(key, part):
    return expert_matrix(key, 11)


def draw_up_weight(key, part):
    return expert_matrix(key, 12)


def draw_tokens(key, part):
    base = jax.random.fold_in(key, 21)
    rough = jnp.exp(jax.random.uniform(jax.random.fold_in(base, 3), (1, D), jnp.float32, -0.35, 0.35))
    rising = 3.0 ** (jnp.arange(D, dtype=jnp.float32)[None, :] / max(D - 1, 1))
    noise = jax.random.truncated_normal(jax.random.fold_in(base, 1), -6.0, 6.0, (TOKENS, D), jnp.float32)
    scales = jnp.exp(jax.random.uniform(jax.random.fold_in(base, 2), (TOKENS, 1), jnp.float32, 0.0, math.log(10.0)))
    return (noise * scales * rising * rough).astype(jnp.bfloat16)


def block_levels(rng, dims, split, smallest, largest):
    loudness = 1.0
    for axis_at, shards_of in split:
        draws = jax.random.uniform(jax.random.fold_in(jax.random.fold_in(rng, 6), axis_at), (shards_of,), jnp.float32, smallest / len(split), largest / len(split))
        loudness = loudness * jnp.repeat(jnp.exp(draws), dims[axis_at] // shards_of).reshape((-1,) + (1,) * (len(dims) - 1 - axis_at))
    return loudness


def assign_block(key, own, number, rows, count, top, bound, skew):
    sequence = jax.random.permutation(key, count)
    packed, ordinary = load_shares(count, rows * top, bound, skew, True), load_shares(count, rows * top, bound, skew, False)
    places = jnp.arange(count)

    def named(sizes, turn):
        used = int((sizes > 0).sum())
        fixed = max(1, used // 4)
        shifted = fixed + (places - fixed + turn * (used - fixed)) % max(1, count - fixed)
        return jnp.zeros((count,), jnp.int32).at[sequence[jnp.where(places < fixed, places, shifted)]].set(jnp.asarray(sizes, jnp.int32))

    sizes = jnp.where(number % 4 == 0, named(packed, number // 4), named(ordinary, number - number // 4 - 1))
    mixed = jax.random.permutation(jax.random.fold_in(own, 3), count)
    source_of, receiver = mixed[0:count // 2 * 2:2], mixed[1:count // 2 * 2:2]
    slack = jnp.minimum(sizes[source_of] - 1, bound - sizes[receiver]) // 2
    slack = jnp.where((source_of == sequence[0]) | (receiver == sequence[0]) | (sizes[receiver] == 0), 0, jnp.maximum(slack, 0))
    shifted = jax.random.randint(jax.random.fold_in(own, 4), (count // 2,), 0, 1 << 20) % (slack + 1)
    sizes = sizes.at[source_of].add(-shifted).at[receiver].add(shifted)
    members = jnp.searchsorted(jnp.cumsum(sizes), jnp.arange(rows * top), side="right").astype(jnp.int32)
    table = members.reshape(top, rows).T
    table = table[jax.random.permutation(jax.random.fold_in(own, 1), rows)]
    turn = jax.random.randint(jax.random.fold_in(own, 2), (rows, 1), 0, top)
    return jnp.take_along_axis(table, (jnp.arange(top)[None, :] + turn) % top, axis=1)


def load_shares(number_of, total, limit, skew, full):
    weights = [(1 << 20) // math.isqrt(rank ** skew) + 1 for rank in range(1, number_of + 1)]
    largest = limit if full else min(limit, max(-(-total // number_of), total * weights[0] // sum(weights)))
    least = 1 if total - largest >= number_of - 1 else 0
    given, rest = [largest] + [least] * (number_of - 1), total - largest - least * (number_of - 1)
    while rest > 0:
        movable = [i for i in range(1, number_of) if given[i] < largest] or [i for i in range(1, number_of) if given[i] < limit]
        pool, budget = sum([weights[i] for i in movable]), rest
        for i in movable:
            more = min(limit - given[i], max(1, budget * weights[i] // pool), rest)
            given[i] = given[i] + more
            rest = rest - more
    return np.array(given)


def gaussian(key, extent, width, bound, cuts=(), held_as=jnp.bfloat16):
    factor_of = block_levels(key, extent, cuts, -0.22, 0.18) if cuts else 1.0
    entries = jax.random.normal(key, extent, jnp.float32) * width * factor_of
    return jnp.minimum(jnp.maximum(entries, -bound), bound).astype(held_as)


def setup_inputs(seed: int = 0) -> dict:
    splits = jax.random.split(jax.random.key(seed), 8)
    tokens = draw_tokens(jax.random.fold_in(splits[7], 71), 0)
    norm_gain = jnp.clip(1.0 + 0.18 * jax.random.normal(splits[1], (D,), jnp.float32), 0.1, 1.9)
    gate_weight = draw_gate_weight(jax.random.fold_in(splits[7], 71), 0)
    up_weight = draw_up_weight(jax.random.fold_in(splits[7], 71), 0)
    down_weight = gaussian(splits[4], (EXPERTS, FF, D), FF ** -0.5, 0.1875, ((1, 16), (2, 2)), jnp.float32)
    routes_keys = jax.random.split(jax.random.fold_in(splits[5], 1), TOKENS // TOK_DEV)
    routes_turns = jax.random.permutation(jax.random.fold_in(splits[5], 3), TOKENS // TOK_DEV)
    routes = jax.vmap(lambda own, number: assign_block(jax.random.fold_in(splits[5], 2), own, number, TOK_DEV, EXPERTS, TOP_K, CAP, 2))(routes_keys, routes_turns).reshape((TOKENS, TOP_K))
    route_weights = jnp.clip(jnp.exp(math.log(1.0) - 2.9957323 * jax.random.uniform(splits[6], (TOKENS, TOP_K), jnp.float32) ** block_levels(splits[6], (TOKENS, TOP_K), ((0, 16),), -0.2, 0.2)), 0.05, 1.0)
    return {"tokens": tokens, "norm_gain": norm_gain, "gate_weight": gate_weight, "up_weight": up_weight, "down_weight": down_weight, "routes": routes, "route_weights": route_weights}


epsilon = 1e-05

def activate(gate_pre, up_pre):
    gated = jnp.minimum(gate_pre, 7.0)
    upper = jnp.clip(up_pre, -7.0, 7.0)
    return (upper + 1.0) * gated * jax.nn.sigmoid(1.702 * gated)

def reference(tokens, norm_gain, gate_weight, up_weight, down_weight, routes, route_weights):
    gate_ready = (norm_gain[None, :, None] * gate_weight).astype(jnp.bfloat16)
    up_ready = (norm_gain[None, :, None] * up_weight).astype(jnp.bfloat16)
    down_ready = down_weight.astype(jnp.bfloat16)
    values = tokens.astype(jnp.float32)
    normed = (values * lax.rsqrt(lax.optimization_barrier(jnp.mean(values * values, axis=1, keepdims=True)) + epsilon)).astype(jnp.bfloat16)
    pairs = TOK_DEV * TOP_K
    chosen = routes.reshape(N_FS, pairs)
    onehot = (chosen[:, :, None] == jnp.arange(EXPERTS, dtype=jnp.int32)[None, None, :]).astype(jnp.int32)
    position = lax.optimization_barrier(jnp.sum(jnp.cumsum(onehot, axis=1) * onehot, axis=2)) - 1
    source = jnp.arange(N_FS, dtype=jnp.int32)[:, None]
    row_index = (source * CAP + position).astype(jnp.int32)
    token_index = (source * TOK_DEV + jnp.arange(pairs, dtype=jnp.int32)[None, :] // TOP_K).astype(jnp.int32)
    table = jnp.zeros((EXPERTS, N_FS * CAP), jnp.int32).at[chosen, row_index].set(token_index)

    def expert(operands):
        indices, gate_mat, up_mat, down_mat = operands
        rows = normed[indices]
        gate_pre = jnp.dot(rows, gate_mat, preferred_element_type=jnp.float32)
        up_pre = jnp.dot(rows, up_mat, preferred_element_type=jnp.float32)
        hidden = activate(gate_pre, up_pre).astype(jnp.bfloat16)
        return jnp.dot(hidden, down_mat, preferred_element_type=jnp.float32).astype(jnp.bfloat16)
    outputs = lax.map(expert, (table, gate_ready, up_ready, down_ready))
    picked = outputs[chosen, row_index].astype(jnp.float32).reshape(TOKENS, TOP_K, D)
    mixed = lax.optimization_barrier(jnp.sum(picked * route_weights[:, :, None], axis=1)).astype(jnp.bfloat16)
    return (mixed, gate_ready, up_ready, down_ready)
```

```python
import math

import jax
import jax.numpy as jnp
from jax import lax
from jax.sharding import PartitionSpec as P

epsilon = 1e-05
bf16 = jnp.bfloat16
f32 = jnp.float32


def activate(gate_pre, up_pre):
    gated = jnp.minimum(gate_pre, 7.0)
    upper = jnp.clip(up_pre, -7.0, 7.0)
    return (upper + 1.0) * gated * jax.nn.sigmoid(1.702 * gated)


def parts_of(weights):
    first = lax.reduce_precision(weights, 8, 7)
    rest = weights - first
    second = lax.reduce_precision(rest, 8, 7)
    return [p.astype(bf16) for p in (first, second, rest - second)]


def over_tp(value):
    size, mine = lax.axis_size("tp"), lax.axis_index("tp")
    blocks = [(mine, value)]
    for j in range(1, size):
        pairs = [(s, (s + j) % size) for s in range(size)]
        blocks.append(((mine - j) % size, lax.ppermute(value, "tp", pairs)))
    return blocks


def product(blocks, matrix):
    total = 0.0
    for owner, value in blocks:
        depth = value.shape[1]
        rows = lax.dynamic_slice_in_dim(matrix, owner * depth, depth, 0)
        total = total + jnp.dot(value, rows, preferred_element_type=f32)
    return total


def shards(tokens, norm_gain, gate_weight, up_weight, down_weight, routes, route_weights):
    count, tp = lax.axis_size("fs"), lax.axis_size("tp")
    inner = math.gcd(count, 4)
    depth = count // inner
    me = lax.axis_index("fs")
    level, place = me // inner, me % inner
    rows, width = tokens.shape
    top = routes.shape[1]
    experts = gate_weight.shape[0]
    capacity = 2 * rows * top // experts

    gate_send = (norm_gain[None, :, None] * gate_weight).astype(bf16)
    up_send = (norm_gain[None, :, None] * up_weight).astype(bf16)
    down_send = down_weight.astype(bf16)
    gate_ready, up_ready, down_ready = (
        lax.all_to_all(sent, "fs", split_axis=0, concat_axis=1, tiled=True)
        for sent in (gate_send, up_send, down_send)
    )

    values = tokens.astype(f32)
    squared = lax.psum(jnp.sum(values * values, axis=1), "tp")
    normed = (values * lax.rsqrt(squared / (width * tp) + epsilon)[:, None]).astype(bf16)
    notes = jnp.concatenate([routes.T.astype(bf16)] + parts_of(route_weights.T), axis=0)
    notes = jnp.concatenate([notes[: 2 * top], notes[2 * top :]], axis=1)
    notes = jnp.pad(notes, ((0, 0), (0, width - 2 * rows)))
    payload = jnp.concatenate([normed, notes], axis=0)

    def shift(value, step, first):
        pairs = []
        for s in range(count):
            at = s // inner
            if 0 <= at + step < depth and (at >= first if step > 0 else at < depth - first):
                pairs.append((s, s + step * inner))
        return lax.ppermute(value, "fs", pairs)

    ups, downs = [payload], [payload]
    for r in range(1, depth):
        ups.append(shift(ups[-1], 1, r - 1))
        downs.append(shift(downs[-1], -1, r - 1))
    column = [payload]
    for q in range(1, depth):
        column.append(jnp.where(level + q < depth, downs[q], ups[depth - q]))
    column = jnp.stack(column)
    column_tokens = column[:, :rows]
    column_notes = column[:, rows:, : 2 * rows].astype(f32)
    column_routes = column_notes[:, :top, :rows]
    column_weights = (
        column_notes[:, top:, :rows] + column_notes[:, :top, rows:] + column_notes[:, top:, rows:]
    )

    targets = level * inner + jnp.bitwise_xor(place, jnp.arange(inner, dtype=jnp.int32))
    named = column_routes[:, None] == targets.astype(f32)[None, :, None, None]
    member = jnp.any(named, axis=2)
    share = jnp.sum(jnp.where(named, column_weights[:, None], 0.0), axis=2)
    before = (jnp.arange(rows)[:, None] < jnp.arange(rows)[None, :]).astype(bf16)
    position = jnp.einsum(
        "qrs,st->qrt", member.astype(bf16), before, preferred_element_type=f32
    )
    slots = jnp.arange(capacity, dtype=jnp.int32).astype(f32)
    chosen = member[:, :, None, :] & (position[:, :, None, :] == slots[None, None, :, None])
    picked = jnp.einsum(
        "qrct,qtd->rqcd", chosen.astype(bf16), column_tokens, preferred_element_type=f32
    ).astype(bf16)
    picked = picked.reshape(inner, depth * capacity, width)

    def swap(value, r):
        if r == 0:
            return value
        return lax.ppermute(value, "fs", [(s, s ^ r) for s in range(count)])

    arrived = jnp.concatenate([swap(picked[r], r) for r in range(inner)], axis=0)
    arrived = over_tp(arrived)
    gate_pre = product(arrived, gate_ready[0])
    up_pre = product(arrived, up_ready[0])
    hidden = over_tp(activate(gate_pre, up_pre).astype(bf16))
    results = product(hidden, down_ready[0]).astype(bf16)
    results = results.reshape(inner, depth * capacity, width)
    back = jnp.stack([swap(results[r], r) for r in range(inner)])
    back = back.reshape(inner, depth, capacity, width)
    scale = jnp.where(chosen, share[:, :, None, :], 0.0)
    partial = jnp.einsum(
        "qrct,rqcd->qtd",
        scale,
        back.astype(f32),
        preferred_element_type=f32,
        precision=lax.Precision.HIGHEST,
    )
    upward, downward = 0.0, 0.0
    for r in range(1, depth):
        def carried(value, step):
            pairs = []
            for s in range(count):
                at = s // inner
                if step > 0 and at + depth - r < depth or step < 0 and at - (depth - r) >= 0:
                    pairs.append((s, s + step * inner))
            return lax.ppermute(value.astype(bf16), "fs", pairs).astype(f32)

        upward = carried(partial[depth - r] + upward, 1)
        downward = carried(partial[r] + downward, -1)
    mixed = (partial[0] + upward + downward).astype(bf16)
    return (mixed, gate_ready, up_ready, down_ready)


def solution(mesh):
    placed = (
        P("fs", "tp"),
        P("fs"),
        P(None, "fs", "tp"),
        P(None, "fs", "tp"),
        P(None, "fs", "tp"),
        P("fs", None),
        P("fs", None),
    )
    return jax.shard_map(
        shards,
        mesh=mesh,
        in_specs=placed,
        out_specs=(P("fs", "tp"), P("fs", None, "tp"), P("fs", None, "tp"), P("fs", None, "tp")),
        check_vma=False,
    )
```

```python
import math

import jax
import jax.numpy as jnp
from jax import lax
from jax.sharding import PartitionSpec as P


epsilon = 1e-05
bf16 = jnp.bfloat16
f32 = jnp.float32


def activate(gate_pre, up_pre):
    gated = jnp.minimum(gate_pre, 7.0)
    upper = jnp.clip(up_pre, -7.0, 7.0)
    return (upper + 1.0) * gated * jax.nn.sigmoid(1.702 * gated)


def parts_of(weights):
    first = lax.reduce_precision(weights, 8, 7)
    rest = weights - first
    second = lax.reduce_precision(rest, 8, 7)
    return [p.astype(bf16) for p in (first, second, rest - second)]


def layout_of(count):
    inner = math.gcd(count, 4)
    return inner, count // inner


def chunks_of(width):
    last = width // 4 if width % 512 == 0 else width // 2
    return [(0, width - last), (width - last, last)]


def far_first(depth):
    return [q for q in range(1, depth) if q != 1] + [1] * (depth > 1)


def over_tp(value):
    size, mine = lax.axis_size("tp"), lax.axis_index("tp")
    blocks = [(mine, value)]
    for j in range(1, size):
        pairs = [(s, (s + j) % size) for s in range(size)]
        blocks.append(((mine - j) % size, lax.ppermute(value, "tp", pairs)))
    return blocks


def product(blocks, matrix):
    total = 0.0
    for owner, value in blocks:
        depth = value.shape[1]
        rows = lax.dynamic_slice_in_dim(matrix, owner * depth, depth, 0)
        total = total + jnp.dot(value, rows, preferred_element_type=f32)
    return total


def take(array, index, axis):
    return lax.dynamic_index_in_dim(array, index, axis, keepdims=False)


def put(array, value, index, axis):
    return lax.dynamic_update_index_in_dim(array, value, index, axis)


def shards(tokens, norm_gain, gate_weight, up_weight, down_weight, routes, route_weights):
    count, tp = lax.axis_size("fs"), lax.axis_size("tp")
    inner, depth = layout_of(count)
    me = lax.axis_index("fs")
    level, place = me // inner, me % inner
    rows, width = tokens.shape
    top = routes.shape[1]
    experts = gate_weight.shape[0]
    capacity = 2 * rows * top // experts
    chunks = chunks_of(width)

    def plane(value, r):
        return lax.ppermute(value, "fs", [(s, s ^ r) for s in range(count)])

    def line(value, q):
        return lax.ppermute(value, "fs", [(s, s ^ (q * inner)) for s in range(count)])

    notes = jnp.concatenate([routes.T.astype(bf16)] + parts_of(route_weights.T), axis=0)
    notes = jnp.concatenate([notes[: 2 * top], notes[2 * top :]], axis=1)
    notes = jnp.pad(notes, ((0, 0), (0, width - 2 * rows)))
    payload = jnp.concatenate([tokens, notes], axis=0)

    def shift(value, step, first):
        pairs = []
        for s in range(count):
            at = s // inner
            if 0 <= at + step < depth and (at >= first if step > 0 else at < depth - first):
                pairs.append((s, s + step * inner))
        return lax.ppermute(value, "fs", pairs)

    ups, downs = [payload], [payload]
    for n in range(1, depth):
        ups.append(shift(ups[-1], 1, n - 1))
        downs.append(shift(downs[-1], -1, n - 1))
    column = [payload]
    for q in range(1, depth):
        column.append(jnp.where(level + q < depth, downs[q], ups[depth - q]))
    column = jnp.stack(column)

    def blocks_of(weight, gain):
        shaped = weight.reshape((depth, inner) + weight.shape[1:])

        def block(index, axis):
            part = take(shaped, index, axis)
            return (part * gain[None, :, None] if gain is not None else part).astype(bf16)

        return block

    def line_then_plane(block):
        stage = jnp.zeros((depth, inner) + block(0, 0).shape[1:], bf16)
        stage = put(stage, block(level, 0), level, 0)
        for q in far_first(depth):
            stage = put(stage, line(block(level ^ q, 0), q), level ^ q, 0)
        out = put(stage, take(stage, place, 1), place, 1)
        for r in range(1, inner):
            got = plane(take(stage, place ^ r, 1), r)
            out = put(out, got, place ^ r, 1)
        return out

    def plane_stage(block):
        stage = jnp.zeros((inner, depth) + block(0, 0).shape[1:], bf16)
        stage = put(stage, block(place, 1), place, 0)
        for r in range(1, inner):
            stage = put(stage, plane(block(place ^ r, 1), r), place ^ r, 0)
        return stage

    def line_stage(stage):
        out = jnp.zeros((depth, inner) + stage.shape[2:], bf16)
        out = put(out, take(stage, level, 1), level, 0)
        for q in far_first(depth):
            got = line(take(stage, level ^ q, 1), q)
            out = put(out, got, level ^ q, 0)
        return out

    gate_out = line_then_plane(blocks_of(gate_weight, norm_gain))
    gate_ready = gate_out.reshape(-1, gate_weight.shape[2])
    up_out = line_stage(plane_stage(blocks_of(up_weight, norm_gain)))
    up_ready = up_out.reshape(-1, up_weight.shape[2])
    down_stage = plane_stage(blocks_of(down_weight, None))
    down_parts = []
    for start, size in chunks:
        part = line_stage(down_stage[..., start : start + size])
        down_parts.append(part.reshape(-1, size))
    down_ready = jnp.concatenate(down_parts, axis=1)

    column_tokens = column[:, :rows]
    column_notes = column[:, rows:, : 2 * rows].astype(f32)
    column_routes = column_notes[:, :top, :rows]
    column_weights = (
        column_notes[:, top:, :rows] + column_notes[:, :top, rows:] + column_notes[:, top:, rows:]
    )
    targets = level * inner + jnp.bitwise_xor(place, jnp.arange(inner, dtype=jnp.int32))
    named = column_routes[:, None] == targets.astype(f32)[None, :, None, None]
    member = jnp.any(named, axis=2)
    share = jnp.sum(jnp.where(named, column_weights[:, None], 0.0), axis=2)
    before = (jnp.arange(rows)[:, None] < jnp.arange(rows)[None, :]).astype(bf16)
    position = jnp.einsum("qrs,st->qrt", member.astype(bf16), before, preferred_element_type=f32)
    slots = jnp.arange(capacity, dtype=jnp.int32).astype(f32)
    chosen = member[:, :, None, :] & (position[:, :, None, :] == slots[None, None, :, None])
    picked = jnp.einsum(
        "qrct,qtd->rqcd", chosen.astype(bf16), column_tokens, preferred_element_type=f32
    ).astype(bf16)
    picked = picked.reshape(inner, depth * capacity, width)

    arrived = [picked[0]] + [plane(picked[r], r) for r in range(1, inner)]
    arrived = over_tp(jnp.concatenate(arrived, axis=0))
    squared = sum(jnp.sum(jnp.square(x.astype(f32)), axis=1, keepdims=True) for _, x in arrived)
    factor = lax.rsqrt(squared / (width * tp) + epsilon)
    normed = [(owner, (x.astype(f32) * factor).astype(bf16)) for owner, x in arrived]
    hidden = activate(product(normed, gate_ready), product(normed, up_ready)).astype(bf16)
    hidden = over_tp(hidden)

    scale = jnp.where(chosen, share[:, :, None, :], 0.0)
    partials = []
    for c, (start, size) in enumerate(chunks):
        results = product(hidden, down_parts[c]).astype(bf16)
        results = results.reshape(inner, depth * capacity, size)
        back = [results[0]] + [plane(results[r], r) for r in range(1, inner)]
        back = jnp.stack(back).reshape(inner, depth, capacity, size)
        partials.append(
            jnp.einsum(
                "qrct,rqcd->qtd",
                scale,
                back.astype(f32),
                preferred_element_type=f32,
                precision=lax.Precision.HIGHEST,
            )
        )
    mixed = []
    for partial in partials:
        upward, downward = 0.0, 0.0
        for n in range(1, depth):
            reach = depth - n
            lift = [(s, s + inner) for s in range(count) if s // inner + reach < depth]
            drop = [(s, s - inner) for s in range(count) if s // inner >= reach]
            upward = lax.ppermute((partial[reach] + upward).astype(bf16), "fs", lift)
            downward = lax.ppermute((partial[n] + downward).astype(bf16), "fs", drop)
            upward, downward = upward.astype(f32), downward.astype(f32)
        mixed.append((partial[0] + upward + downward).astype(bf16))
    mixed = jnp.concatenate(mixed, axis=1)
    return (mixed, gate_ready[None], up_ready[None], down_ready[None])


def solution(mesh):
    placed = (
        P("fs", "tp"),
        P("fs"),
        P(None, "fs", "tp"),
        P(None, "fs", "tp"),
        P(None, "fs", "tp"),
        P("fs", None),
        P("fs", None),
    )

    def program(*arrays):
        return jax.shard_map(
            shards,
            mesh=mesh,
            in_specs=placed,
            out_specs=(P("fs", "tp"), P("fs", None, "tp"), P("fs", None, "tp"), P("fs", None, "tp")),
            check_vma=False,
        )(*arrays)

    return program
```

```python
import math

import jax
import jax.numpy as jnp
from jax import lax
from jax.sharding import PartitionSpec as P


epsilon = 1e-05
bf16 = jnp.bfloat16
f32 = jnp.float32


def activate(gate_pre, up_pre):
    gated = jnp.minimum(gate_pre, 7.0)
    upper = jnp.clip(up_pre, -7.0, 7.0)
    return (upper + 1.0) * gated * jax.nn.sigmoid(1.702 * gated)


def parts_of(weights):
    first = lax.reduce_precision(weights, 8, 7)
    rest = weights - first
    second = lax.reduce_precision(rest, 8, 7)
    return [p.astype(bf16) for p in (first, second, rest - second)]


def layout_of(count):
    inner = math.gcd(count, 4)
    return inner, count // inner


def chunks_of(width):
    unit = width // 4
    return [(0, 2 * unit), (2 * unit, unit), (3 * unit, width - 3 * unit)]


def far_first(depth):
    return [q for q in range(1, depth) if q != 1] + [1] * (depth > 1)


def after(value, *others):
    return lax.optimization_barrier((value,) + others)[0]


def over_tp(value):
    size, mine = lax.axis_size("tp"), lax.axis_index("tp")
    blocks = [(mine, value)]
    for j in range(1, size):
        pairs = [(s, (s + j) % size) for s in range(size)]
        blocks.append(((mine - j) % size, lax.ppermute(value, "tp", pairs)))
    return blocks


def product(blocks, matrix):
    total = 0.0
    for owner, value in blocks:
        depth = value.shape[1]
        rows = lax.dynamic_slice_in_dim(matrix, owner * depth, depth, 0)
        total = total + jnp.dot(value, rows, preferred_element_type=f32)
    return total


def take(array, index, axis):
    return lax.dynamic_index_in_dim(array, index, axis, keepdims=False)


def put(array, value, index, axis):
    return lax.dynamic_update_index_in_dim(array, value, index, axis)


def shards(tokens, norm_gain, gate_weight, up_weight, down_weight, routes, route_weights):
    count, tp = lax.axis_size("fs"), lax.axis_size("tp")
    inner, depth = layout_of(count)
    me = lax.axis_index("fs")
    level, place = me // inner, me % inner
    rows, width = tokens.shape
    top = routes.shape[1]
    experts = gate_weight.shape[0]
    capacity = 2 * rows * top // experts
    chunks = chunks_of(width)

    def plane(value, r):
        return lax.ppermute(value, "fs", [(s, s ^ r) for s in range(count)])

    def line(value, q):
        return lax.ppermute(value, "fs", [(s, s ^ (q * inner)) for s in range(count)])

    notes = jnp.concatenate([routes.T.astype(bf16)] + parts_of(route_weights.T), axis=0)
    notes = jnp.concatenate([notes[: 2 * top], notes[2 * top :]], axis=1)
    notes = jnp.pad(notes, ((0, 0), (0, width - 2 * rows)))
    payload = jnp.concatenate([tokens, notes], axis=0)

    def shift(value, step, first):
        pairs = []
        for s in range(count):
            at = s // inner
            if 0 <= at + step < depth and (at >= first if step > 0 else at < depth - first):
                pairs.append((s, s + step * inner))
        return lax.ppermute(value, "fs", pairs)

    ups, downs = [payload], [payload]
    for n in range(1, depth):
        ups.append(shift(ups[-1], 1, n - 1))
        downs.append(shift(downs[-1], -1, n - 1))
    column = [payload]
    for q in range(1, depth):
        block = payload
        for offset in sorted({(at ^ q) - at for at in range(depth)}):
            held = downs[offset] if offset > 0 else ups[-offset]
            block = jnp.where((level ^ q) - level == offset, held, block)
        column.append(block)
    column = jnp.stack(column)

    def blocks_of(weight, gain):
        shaped = weight.reshape((depth, inner) + weight.shape[1:])

        def block(index, axis):
            part = take(shaped, index, axis)
            return (part * gain[None, :, None] if gain is not None else part).astype(bf16)

        return block

    def chained(block, axis, indices, held):
        made = []
        for index in indices:
            made.append(block(after(index, held), axis))
            held = made[-1]
        return made

    line_order, plane_order = far_first(depth), list(range(1, inner))

    def line_then_plane(block):
        made = [block(level ^ line_order[0], 0)] if depth > 1 else []
        rest = [level ^ q for q in line_order[1:]] + [level]
        made += chained(block, 0, rest, ups[min(1, depth - 1)])
        stage = jnp.zeros((depth, inner) + made[0].shape[1:], bf16)
        stage = put(stage, made[-1], level, 0)
        for q, piece in zip(line_order, made):
            stage = put(stage, line(piece, q), level ^ q, 0)
        out = put(stage, take(stage, place, 1), place, 1)
        for r in range(1, inner):
            got = plane(take(stage, place ^ r, 1), r)
            out = put(out, got, place ^ r, 1)
        return out, made[0]

    def plane_stage(block, held):
        made = chained(block, 1, [place ^ r for r in plane_order] + [place], held)
        stage = jnp.zeros((inner, depth) + made[0].shape[1:], bf16)
        stage = put(stage, made[-1], place, 0)
        for r, piece in zip(plane_order, made):
            stage = put(stage, plane(piece, r), place ^ r, 0)
        return stage

    def line_parts(stage):
        return [take(stage, level, 1)] + [line(take(stage, level ^ q, 1), q) for q in line_order]

    def joined(parts, held=None):
        out = jnp.zeros((depth,) + parts[0].shape, bf16)
        for q, part in zip([0] + line_order, parts):
            index = level ^ q if held is None else after(level ^ q, held)
            out = put(out, part, index, 0)
        return out.reshape(-1, parts[0].shape[-1])

    gate_out, first_sent = line_then_plane(blocks_of(gate_weight, norm_gain))
    gate_ready = gate_out.reshape(-1, gate_weight.shape[2])
    up_stage = plane_stage(blocks_of(up_weight, norm_gain), first_sent)
    up_ready = joined(line_parts(up_stage))
    down_stage = plane_stage(blocks_of(down_weight, None), up_stage)
    down_parts = [line_parts(down_stage[..., start : start + size]) for start, size in chunks]

    column_tokens = column[:, :rows]
    column_notes = column[:, rows:, : 2 * rows].astype(f32)
    column_routes = column_notes[:, :top, :rows]
    column_weights = (
        column_notes[:, top:, :rows] + column_notes[:, :top, rows:] + column_notes[:, top:, rows:]
    )
    targets = level * inner + jnp.bitwise_xor(place, jnp.arange(inner, dtype=jnp.int32))
    named = column_routes[:, None] == targets.astype(f32)[None, :, None, None]
    member = jnp.any(named, axis=2)
    share = jnp.sum(jnp.where(named, column_weights[:, None], 0.0), axis=2)
    before = (jnp.arange(rows)[:, None] < jnp.arange(rows)[None, :]).astype(bf16)
    position = jnp.einsum("qrs,st->qrt", member.astype(bf16), before, preferred_element_type=f32)
    slots = jnp.arange(capacity, dtype=jnp.int32).astype(f32)
    chosen = member[:, :, None, :] & (position[:, :, None, :] == slots[None, None, :, None])
    picked = jnp.einsum(
        "qrct,qtd->rqcd", chosen.astype(bf16), column_tokens, preferred_element_type=f32
    ).astype(bf16)
    picked = picked.reshape(inner, depth * capacity, width)

    arrived = [picked[0]] + [plane(picked[r], r) for r in range(1, inner)]
    arrived = over_tp(jnp.concatenate(arrived, axis=0))
    squared = sum(jnp.sum(jnp.square(x.astype(f32)), axis=1, keepdims=True) for _, x in arrived)
    factor = lax.rsqrt(squared / (width * tp) + epsilon)
    normed = [(owner, (x.astype(f32) * factor).astype(bf16)) for owner, x in arrived]
    hidden = activate(product(normed, gate_ready), product(normed, up_ready)).astype(bf16)
    hidden = over_tp(hidden)

    scale = jnp.where(chosen, share[:, :, None, :], 0.0)
    partials, down_ready, held = [], [], hidden[-1][1]
    for c, (start, size) in enumerate(chunks):
        down_ready.append(joined(down_parts[c], held))
        results = product(hidden, down_ready[c]).astype(bf16)
        held = results
        results = results.reshape(inner, depth * capacity, size)
        back = [results[0]] + [plane(results[r], r) for r in range(1, inner)]
        back = jnp.stack(back).reshape(inner, depth, capacity, size)
        partials.append(
            jnp.einsum(
                "qrct,rqcd->qtd",
                scale,
                back.astype(f32),
                preferred_element_type=f32,
                precision=lax.Precision.HIGHEST,
            )
        )
    mixed = []
    for partial in partials:
        total = partial[0]
        for q in line_order:
            total = total + line(partial[q].astype(bf16), q).astype(f32)
        mixed.append(total.astype(bf16))
    mixed = jnp.concatenate(mixed, axis=1)
    down_ready = jnp.concatenate(down_ready, axis=1)
    return (mixed, gate_ready[None], up_ready[None], down_ready[None])


def solution(mesh):
    placed = (
        P("fs", "tp"),
        P("fs"),
        P(None, "fs", "tp"),
        P(None, "fs", "tp"),
        P(None, "fs", "tp"),
        P("fs", None),
        P("fs", None),
    )

    def program(*arrays):
        return jax.shard_map(
            shards,
            mesh=mesh,
            in_specs=placed,
            out_specs=(P("fs", "tp"), P("fs", None, "tp"), P("fs", None, "tp"), P("fs", None, "tp")),
            check_vma=False,
        )(*arrays)

    return program
```

```python
import math

import jax
import jax.numpy as jnp
from jax import lax
from jax.sharding import PartitionSpec as P


epsilon = 1e-05
bf16 = jnp.bfloat16
f32 = jnp.float32


def activate(gate_pre, up_pre):
    gated = jnp.minimum(gate_pre, 7.0)
    upper = jnp.clip(up_pre, -7.0, 7.0)
    return (upper + 1.0) * gated * jax.nn.sigmoid(1.702 * gated)


def parts_of(weights):
    first = lax.reduce_precision(weights, 8, 7)
    rest = weights - first
    second = lax.reduce_precision(rest, 8, 7)
    return [p.astype(bf16) for p in (first, second, rest - second)]


def layout_of(count):
    inner = math.gcd(count, 4)
    return inner, count // inner


def chunks_of(width):
    unit = width // 4
    return [(0, 2 * unit), (2 * unit, unit), (3 * unit, width - 3 * unit)]


def far_first(depth):
    return [q for q in range(1, depth) if q != 1] + [1] * (depth > 1)


def after(value, *others):
    return lax.optimization_barrier((value,) + others)[0]


def over_tp(value):
    size, mine = lax.axis_size("tp"), lax.axis_index("tp")
    blocks = [(mine, value)]
    for j in range(1, size):
        pairs = [(s, (s + j) % size) for s in range(size)]
        blocks.append(((mine - j) % size, lax.ppermute(value, "tp", pairs)))
    return blocks


def product(blocks, matrix):
    total = 0.0
    for owner, value in blocks:
        depth = value.shape[1]
        rows = lax.dynamic_slice_in_dim(matrix, owner * depth, depth, 0)
        total = total + jnp.dot(value, rows, preferred_element_type=f32)
    return total


def take(array, index, axis):
    return lax.dynamic_index_in_dim(array, index, axis, keepdims=False)


def put(array, value, index, axis):
    return lax.dynamic_update_index_in_dim(array, value, index, axis)


def shards(tokens, norm_gain, gate_weight, up_weight, down_weight, routes, route_weights):
    count, tp = lax.axis_size("fs"), lax.axis_size("tp")
    inner, depth = layout_of(count)
    me = lax.axis_index("fs")
    level, place = me // inner, me % inner
    rows, width = tokens.shape
    top = routes.shape[1]
    experts = gate_weight.shape[0]
    capacity = 2 * rows * top // experts
    chunks = chunks_of(width)

    def plane(value, r):
        return lax.ppermute(value, "fs", [(s, s ^ r) for s in range(count)])

    def line(value, q):
        return lax.ppermute(value, "fs", [(s, s ^ (q * inner)) for s in range(count)])

    notes = jnp.concatenate([routes.T.astype(bf16)] + parts_of(route_weights.T), axis=0)
    notes = jnp.concatenate([notes[: 2 * top], notes[2 * top :]], axis=1)
    notes = jnp.pad(notes, ((0, 0), (0, width - 2 * rows)))
    payload = jnp.concatenate([tokens, notes], axis=0)

    def shift(value, step, first):
        pairs = []
        for s in range(count):
            at = s // inner
            if 0 <= at + step < depth and (at >= first if step > 0 else at < depth - first):
                pairs.append((s, s + step * inner))
        return lax.ppermute(value, "fs", pairs)

    ups, downs = [payload], [payload]
    for n in range(1, depth):
        ups.append(shift(ups[-1], 1, n - 1))
        downs.append(shift(downs[-1], -1, n - 1))

    line_order, plane_order = far_first(depth), list(range(1, inner))

    def shaped(weight):
        return weight.reshape((depth, inner) + weight.shape[1:])

    def block(weight, gain, index, axis, held):
        if held is not None:
            index = after(index, held)
        part = take(shaped(weight), index, axis)
        return (part * gain[None, :, None] if gain is not None else part).astype(bf16)

    held, gate_sent, up_sent, down_sent = None, {}, {}, {}
    for q in line_order[:1]:
        held = gate_sent[q] = block(gate_weight, norm_gain, level ^ q, 0, held)
    for r in plane_order:
        held = up_sent[r] = block(up_weight, norm_gain, place ^ r, 1, held)
    for q in line_order[1:]:
        held = gate_sent[q] = block(gate_weight, norm_gain, level ^ q, 0, held)
    for r in plane_order:
        held = down_sent[r] = block(down_weight, None, place ^ r, 1, held)
    held = gate_sent[0] = block(gate_weight, norm_gain, level, 0, held)
    held = up_sent[0] = block(up_weight, norm_gain, place, 1, held)
    held = down_sent[0] = block(down_weight, None, place, 1, held)

    gate_got = {q: line(gate_sent[q], q) for q in line_order}
    up_got = {r: plane(up_sent[r], r) for r in plane_order}
    down_got = {r: plane(down_sent[r], r) for r in plane_order}

    def gathered(own, got, at):
        stage = jnp.zeros((len(got) + 1,) + own.shape, bf16)
        stage = put(stage, own, at, 0)
        for step, piece in got.items():
            stage = put(stage, piece, at ^ step, 0)
        return stage

    up_stage = gathered(up_sent[0], up_got, place)
    up_parts = {q: take(up_stage, level ^ q, 1) for q in [0] + line_order}
    for q in line_order:
        up_parts[q] = line(up_parts[q], q)
    down_stage = gathered(down_sent[0], down_got, place)
    down_parts = [
        {
            q: take(down_stage[..., start : start + size], level ^ q, 1)
            for q in [0] + line_order
        }
        for start, size in chunks
    ]
    for c in range(len(chunks)):
        for q in line_order:
            down_parts[c][q] = line(down_parts[c][q], q)

    column = [payload]
    for q in range(1, depth):
        chosen = payload
        for offset in sorted({(at ^ q) - at for at in range(depth)}):
            other = downs[offset] if offset > 0 else ups[-offset]
            chosen = jnp.where((level ^ q) - level == offset, other, chosen)
        column.append(chosen)
    column = jnp.stack(column)
    column_tokens = column[:, :rows]
    column_notes = column[:, rows:, : 2 * rows].astype(f32)
    column_routes = column_notes[:, :top, :rows]
    column_weights = (
        column_notes[:, top:, :rows]
        + column_notes[:, :top, rows:]
        + column_notes[:, top:, rows:]
    )
    targets = level * inner + jnp.bitwise_xor(place, jnp.arange(inner, dtype=jnp.int32))
    named = column_routes[:, None] == targets.astype(f32)[None, :, None, None]
    member = jnp.any(named, axis=2)
    share = jnp.sum(jnp.where(named, column_weights[:, None], 0.0), axis=2)
    before = (jnp.arange(rows)[:, None] < jnp.arange(rows)[None, :]).astype(bf16)
    position = jnp.einsum("qrs,st->qrt", member.astype(bf16), before, preferred_element_type=f32)
    slots = jnp.arange(capacity, dtype=jnp.int32).astype(f32)
    chosen = member[:, :, None, :] & (position[:, :, None, :] == slots[None, None, :, None])
    picked = jnp.einsum(
        "qrct,qtd->rqcd", chosen.astype(bf16), column_tokens, preferred_element_type=f32
    ).astype(bf16)
    picked = picked.reshape(inner, depth * capacity, width)
    scale = jnp.where(chosen, share[:, :, None, :], 0.0)
    arrived = [picked[0]] + [plane(picked[r], r) for r in plane_order]

    gate_stage = gathered(gate_sent[0], gate_got, level)
    gate_parts = {r: take(gate_stage, place ^ r, 1) for r in [0] + plane_order}
    for r in plane_order:
        gate_parts[r] = plane(gate_parts[r], r)

    arrived = jnp.concatenate(arrived, axis=0)
    arrived = over_tp(arrived)
    squared = sum(
        jnp.sum(jnp.square(x.astype(f32)), axis=1, keepdims=True) for _, x in arrived
    )
    factor = lax.rsqrt(squared / (width * tp) + epsilon)
    normed = [(owner, (x.astype(f32) * factor).astype(bf16)) for owner, x in arrived]
    own = up_parts.pop(0)
    up_ready = gathered(own, up_parts, level).reshape(-1, up_weight.shape[2])
    own = gate_parts.pop(0)
    gate_ready = jnp.zeros((depth, inner) + own.shape[1:], bf16)
    gate_ready = put(gate_ready, own, place, 1)
    for r in plane_order:
        gate_ready = put(gate_ready, gate_parts[r], place ^ r, 1)
    gate_ready = gate_ready.reshape(-1, gate_weight.shape[2])
    hidden = activate(product(normed, gate_ready), product(normed, up_ready)).astype(bf16)
    hidden = over_tp(hidden)
    whole = []
    for owner in range(tp):
        piece = hidden[0][1]
        for other, value in hidden[1:]:
            piece = jnp.where(other == owner, value, piece)
        whole.append(piece)
    whole = jnp.concatenate(whole, axis=1)
    unit = whole.shape[1] // depth
    hidden_order = [0] + line_order
    hidden = jnp.concatenate(
        [lax.dynamic_slice_in_dim(whole, (level ^ q) * unit, unit, 1) for q in hidden_order],
        axis=1,
    )

    backs, held = [], None
    for c, (start, size) in enumerate(chunks):
        matrix = jnp.concatenate(
            [down_parts[c][q].reshape(unit, size) for q in hidden_order], axis=0
        )
        results = jnp.dot(hidden, matrix, preferred_element_type=f32).astype(bf16)
        results = results.reshape(inner, depth * capacity, size)
        backs.append([results[0]] + [plane(results[r], r) for r in plane_order])
    sums = []
    for c, (start, size) in enumerate(chunks):
        if held is not None:
            backs[c][0] = after(backs[c][0], held)
        back = jnp.stack(backs[c]).reshape(inner, depth, capacity, size)
        partial = jnp.einsum(
            "qrct,rqcd->qtd",
            scale,
            back.astype(f32),
            preferred_element_type=f32,
            precision=lax.Precision.HIGHEST,
        )
        leaving = {q: partial[q].astype(bf16) for q in line_order}
        held = leaving
        sums.append([partial[0]] + [line(leaving[q], q).astype(f32) for q in line_order])
    down_ready = []
    for c, (start, size) in enumerate(chunks):
        own = down_parts[c].pop(0)
        down_ready.append(gathered(own, down_parts[c], level).reshape(-1, size))
    down_ready = jnp.concatenate(down_ready, axis=1)
    mixed = []
    for c in range(len(chunks)):
        mixed.append(sum(sums[c]).astype(bf16))
    mixed = jnp.concatenate(mixed, axis=1)
    return (mixed, gate_ready[None], up_ready[None], down_ready[None])


def solution(mesh):
    placed = (
        P("fs", "tp"),
        P("fs"),
        P(None, "fs", "tp"),
        P(None, "fs", "tp"),
        P(None, "fs", "tp"),
        P("fs", None),
        P("fs", None),
    )

    def program(*arrays):
        return jax.shard_map(
            shards,
            mesh=mesh,
            in_specs=placed,
            out_specs=(P("fs", "tp"), P("fs", None, "tp"), P("fs", None, "tp"), P("fs", None, "tp")),
            check_vma=False,
        )(*arrays)

    return program
```

```python
import functools
import math

import jax
import jax.numpy as jnp
from jax import lax
from jax.experimental import pallas as pl
from jax.experimental.pallas import tpu as pltpu
from jax.sharding import PartitionSpec as P


epsilon = 1e-05
bf16 = jnp.bfloat16
f32 = jnp.float32


def activate(gate_pre, up_pre):
    gated = jnp.minimum(gate_pre, 7.0)
    upper = jnp.clip(up_pre, -7.0, 7.0)
    return (upper + 1.0) * gated * jax.nn.sigmoid(1.702 * gated)


def parts_of(weights):
    first = lax.reduce_precision(weights, 8, 7)
    rest = weights - first
    second = lax.reduce_precision(rest, 8, 7)
    return [p.astype(bf16) for p in (first, second, rest - second)]


def layout_of(count):
    inner = math.gcd(count, 4)
    return inner, count // inner


def chunks_of(width):
    unit = max(width // 4, math.gcd(width, 128))
    first = max(width // 2, unit)
    return [(0, first)] + [(at, unit) for at in range(first, width, unit)]


def far_first(depth):
    return [q for q in range(1, depth) if q != 1] + [1] * (depth > 1)


def after(value, *others):
    return lax.optimization_barrier((value,) + others)[0]


def over_tp(value):
    size = lax.axis_size("tp")
    blocks = [value]
    for j in range(1, size):
        pairs = [(s, (s + j) % size) for s in range(size)]
        blocks.append(lax.ppermute(value, "tp", pairs))
    return blocks


def spot(index, size):
    return pl.ds(pl.multiple_of(index * size, size), size)


def hidden_kernel(inner, depth, tp, line_order, *refs):
    at, refs = refs[0], list(refs[1:])
    level, place, mine = at[0], at[1], at[2]
    xs, refs = refs[:tp], refs[tp:]
    gates, refs = refs[:inner], refs[inner:]
    ups, refs = refs[:depth], refs[depth:]
    hidden, gate_out, up_out, gate, up, sems = refs
    block = gates[0].shape[1]
    for r in range(inner):
        for level_at in range(depth):
            gate[spot(level_at * inner + (place ^ r), block), :] = gates[r][level_at]
    for q, piece in zip([0] + line_order, ups):
        rows = piece.shape[0] * piece.shape[1]
        up[spot(level ^ q, rows), :] = piece[...].reshape(rows, piece.shape[2])
    width = xs[0].shape[1]
    tile = math.gcd(xs[0].shape[0], 256)

    @pl.loop(0, xs[0].shape[0] // tile)
    def _(step):
        rows = spot(step, tile)
        squared = 0.0
        for x in xs:
            value = x[rows, :].astype(f32)
            squared = squared + jnp.sum(value * value, axis=1, keepdims=True)
        factor = lax.rsqrt(squared / (width * tp) + epsilon)
        gate_pre, up_pre = 0.0, 0.0
        for j, x in enumerate(xs):
            normed = (x[rows, :].astype(f32) * factor).astype(bf16)
            held = spot(lax.rem(mine - j + tp, tp), width)
            gate_pre = gate_pre + jnp.dot(normed, gate[held, :], preferred_element_type=f32)
            up_pre = up_pre + jnp.dot(normed, up[held, :], preferred_element_type=f32)
        hidden[rows, :] = activate(gate_pre, up_pre).astype(bf16)

    copies = [
        pltpu.make_async_copy(gate, gate_out, sems.at[0]),
        pltpu.make_async_copy(up, up_out, sems.at[1]),
    ]
    for copy in copies:
        copy.start()
    for copy in copies:
        copy.wait()


def hidden_call(where, xs, gates, ups, line_order, depth_rows):
    inner, depth, tp = len(gates), len(ups), len(xs)
    columns = gates[0].shape[2]
    rows = xs[0].shape[0]
    vmem = pl.BlockSpec(memory_space=pltpu.VMEM)
    matrix = jax.ShapeDtypeStruct((depth_rows, columns), bf16)
    return pl.pallas_call(
        functools.partial(hidden_kernel, inner, depth, tp, line_order),
        out_shape=(jax.ShapeDtypeStruct((rows, columns), bf16), matrix, matrix),
        in_specs=[pl.BlockSpec(memory_space=pltpu.SMEM)] + [vmem] * (tp + inner + depth),
        out_specs=(vmem, pl.BlockSpec(memory_space=pl.ANY), pl.BlockSpec(memory_space=pl.ANY)),
        scratch_shapes=[
            pltpu.VMEM((depth_rows, columns), bf16),
            pltpu.VMEM((depth_rows, columns), bf16),
            pltpu.SemaphoreType.DMA((2,)),
        ],
        compiler_params=pltpu.CompilerParams(vmem_limit_bytes=28 << 20),
        cost_estimate=pl.CostEstimate(
            flops=4 * rows * depth_rows * columns,
            bytes_accessed=4 * rows * depth_rows,
            transcendentals=rows * columns,
        ),
        name="hidden",
    )(where, *xs, *gates, *ups)


def result_kernel(inner, depth, tp, line_order, start, again, *refs):
    at, refs = refs[0], list(refs[1:])
    level, mine = at[0], at[2]
    hiddens, refs = refs[:tp], refs[tp:]
    parts, refs = refs[:depth], refs[depth + again :]
    results, (down_out, matrix, sem) = refs[:inner], refs[inner:]
    for q, part in zip([0] + line_order, parts):
        rows = part.shape[0] * part.shape[1]
        matrix[spot(level ^ q, rows), :] = part[...].reshape(rows, part.shape[2])
    width, rows = hiddens[0].shape[1], results[0].shape[0]
    for r in range(inner):
        total = 0.0
        for j, hidden in enumerate(hiddens):
            held = matrix[spot(lax.rem(mine - j + tp, tp), width), :]
            total = total + jnp.dot(
                hidden[pl.ds(r * rows, rows), :], held, preferred_element_type=f32
            )
        results[r][...] = total.astype(bf16)
    copy = pltpu.make_async_copy(matrix, down_out.at[:, pl.ds(start, matrix.shape[1])], sem)
    copy.start()
    copy.wait()


def result_call(where, hiddens, parts, before, start, full, inner, line_order):
    depth, tp = len(parts), len(hiddens)
    rows, columns = hiddens[0].shape[0], parts[0].shape[2]
    vmem, anywhere = (pl.BlockSpec(memory_space=m) for m in (pltpu.VMEM, pl.ANY))
    again = int(before is not None)
    piece = jax.ShapeDtypeStruct((rows // inner, columns), bf16)
    return pl.pallas_call(
        functools.partial(result_kernel, inner, depth, tp, line_order, start, again),
        out_shape=(piece,) * inner + (jax.ShapeDtypeStruct(full, bf16),),
        in_specs=[pl.BlockSpec(memory_space=pltpu.SMEM)]
        + [vmem] * (tp + depth)
        + [anywhere] * again,
        out_specs=(vmem,) * inner + (anywhere,),
        scratch_shapes=[pltpu.VMEM((full[0], columns), bf16), pltpu.SemaphoreType.DMA],
        input_output_aliases={1 + tp + depth: inner} if again else {},
        compiler_params=pltpu.CompilerParams(vmem_limit_bytes=16 << 20),
        cost_estimate=pl.CostEstimate(
            flops=2 * rows * full[0] * columns, bytes_accessed=4 * rows * columns, transcendentals=0
        ),
    )(where, *hiddens, *parts, *([before] if again else []))


def take(array, index, axis):
    return lax.dynamic_index_in_dim(array, index, axis, keepdims=False)


def put(array, value, index, axis):
    return lax.dynamic_update_index_in_dim(array, value, index, axis)


def shards(tokens, norm_gain, gate_weight, up_weight, down_weight, routes, route_weights):
    count, tp = lax.axis_size("fs"), lax.axis_size("tp")
    inner, depth = layout_of(count)
    me = lax.axis_index("fs")
    level, place = me // inner, me % inner
    rows, width = tokens.shape
    top = routes.shape[1]
    experts = gate_weight.shape[0]
    capacity = 2 * rows * top // experts
    chunks = chunks_of(width)

    def plane(value, r):
        return lax.ppermute(value, "fs", [(s, s ^ r) for s in range(count)])

    def line(value, q):
        return lax.ppermute(value, "fs", [(s, s ^ (q * inner)) for s in range(count)])

    notes = jnp.concatenate([routes.T.astype(bf16)] + parts_of(route_weights.T), axis=0)
    notes = jnp.concatenate([notes[: 2 * top], notes[2 * top :]], axis=1)
    notes = jnp.pad(notes, ((0, 0), (0, width - 2 * rows)))
    payload = jnp.concatenate([tokens, notes], axis=0)

    def shift(value, step, first):
        pairs = []
        for s in range(count):
            at = s // inner
            if 0 <= at + step < depth and (at >= first if step > 0 else at < depth - first):
                pairs.append((s, s + step * inner))
        return lax.ppermute(value, "fs", pairs)

    ups, downs = [payload], [payload]
    for n in range(1, depth):
        ups.append(shift(ups[-1], 1, n - 1))
        downs.append(shift(downs[-1], -1, n - 1))

    line_order, plane_order = far_first(depth), list(range(1, inner))

    def shaped(weight):
        return weight.reshape((depth, inner) + weight.shape[1:])

    def block(weight, gain, index, axis, held):
        if held is not None:
            index = after(index, held)
        part = take(shaped(weight), index, axis)
        return (part * gain[None, :, None] if gain is not None else part).astype(bf16)

    held, gate_sent, up_sent, down_sent = None, {}, {}, {}
    for q in line_order[:1]:
        held = gate_sent[q] = block(gate_weight, norm_gain, level ^ q, 0, held)
    for r in plane_order:
        held = up_sent[r] = block(up_weight, norm_gain, place ^ r, 1, held)
    for q in line_order[1:]:
        held = gate_sent[q] = block(gate_weight, norm_gain, level ^ q, 0, held)
    for r in plane_order:
        held = down_sent[r] = block(down_weight, None, place ^ r, 1, held)
    held = gate_sent[0] = block(gate_weight, norm_gain, level, 0, held)
    held = up_sent[0] = block(up_weight, norm_gain, place, 1, held)
    held = down_sent[0] = block(down_weight, None, place, 1, held)

    gate_got = {q: line(gate_sent[q], q) for q in line_order}
    up_got = {r: plane(up_sent[r], r) for r in plane_order}
    down_got = {r: plane(down_sent[r], r) for r in plane_order}

    def gathered(own, got, at):
        stage = jnp.zeros((len(got) + 1,) + own.shape, bf16)
        stage = put(stage, own, at, 0)
        for step, piece in got.items():
            stage = put(stage, piece, at ^ step, 0)
        return stage

    up_stage = gathered(up_sent[0], up_got, place)
    up_parts = {q: take(up_stage, level ^ q, 1) for q in [0] + line_order}
    for q in line_order:
        up_parts[q] = line(up_parts[q], q)
    down_stage = gathered(down_sent[0], down_got, place)
    down_parts = [
        {
            q: take(down_stage[..., start : start + size], level ^ q, 1)
            for q in [0] + line_order
        }
        for start, size in chunks
    ]
    for c in range(len(chunks)):
        for q in line_order:
            down_parts[c][q] = line(down_parts[c][q], q)

    column = [payload]
    for q in range(1, depth):
        chosen = payload
        for offset in sorted({(at ^ q) - at for at in range(depth)}):
            other = downs[offset] if offset > 0 else ups[-offset]
            chosen = jnp.where((level ^ q) - level == offset, other, chosen)
        column.append(chosen)
    column = jnp.stack(column)
    column_tokens = column[:, :rows]
    column_notes = column[:, rows:, : 2 * rows].astype(f32)
    column_routes = column_notes[:, :top, :rows]
    column_weights = (
        column_notes[:, top:, :rows]
        + column_notes[:, :top, rows:]
        + column_notes[:, top:, rows:]
    )
    targets = level * inner + jnp.bitwise_xor(place, jnp.arange(inner, dtype=jnp.int32))
    named = column_routes[:, None] == targets.astype(f32)[None, :, None, None]
    member = jnp.any(named, axis=2)
    share = jnp.sum(jnp.where(named, column_weights[:, None], 0.0), axis=2)
    before = (jnp.arange(rows)[:, None] < jnp.arange(rows)[None, :]).astype(bf16)
    position = jnp.einsum("qrs,st->qrt", member.astype(bf16), before, preferred_element_type=f32)
    slots = jnp.arange(capacity, dtype=jnp.int32).astype(f32)
    chosen = member[:, :, None, :] & (position[:, :, None, :] == slots[None, None, :, None])
    picked = jnp.einsum(
        "qrct,qtd->rqcd", chosen.astype(bf16), column_tokens, preferred_element_type=f32
    ).astype(bf16)
    picked = picked.reshape(inner, depth * capacity, width)
    scale = jnp.where(chosen, share[:, :, None, :], 0.0)
    arrived = [picked[0]] + [plane(picked[r], r) for r in plane_order]

    gate_stage = gathered(gate_sent[0], gate_got, level)
    gate_parts = {r: take(gate_stage, place ^ r, 1) for r in [0] + plane_order}
    for r in plane_order:
        gate_parts[r] = plane(gate_parts[r], r)

    arrived = jnp.concatenate(arrived, axis=0)
    arrived = over_tp(arrived)
    spots = jnp.stack([level, place, lax.axis_index("tp")]).astype(jnp.int32)
    hidden, gate_ready, up_ready = hidden_call(
        spots,
        arrived,
        [gate_parts[r] for r in [0] + plane_order],
        [up_parts[q] for q in [0] + line_order],
        line_order,
        width * tp,
    )
    hidden = over_tp(hidden)

    backs, held, down_ready = [], None, None
    for c, (start, size) in enumerate(chunks):
        *results, down_ready = result_call(
            spots,
            hidden,
            [down_parts[c][q] for q in [0] + line_order],
            down_ready,
            start,
            (hidden[0].shape[1] * tp, width),
            inner,
            line_order,
        )
        backs.append([results[0]] + [plane(results[r], r) for r in plane_order])
    sums = []
    for c, (start, size) in enumerate(chunks):
        if held is not None:
            backs[c][0] = after(backs[c][0], held)
        back = jnp.stack(backs[c]).reshape(inner, depth, capacity, size)
        partial = jnp.einsum(
            "qrct,rqcd->qtd",
            scale,
            back.astype(f32),
            preferred_element_type=f32,
            precision=lax.Precision.HIGHEST,
        )
        leaving = {q: partial[q].astype(bf16) for q in line_order}
        held = leaving
        sums.append([partial[0]] + [line(leaving[q], q).astype(f32) for q in line_order])
    mixed = []
    for c in range(len(chunks)):
        mixed.append(sum(sums[c]).astype(bf16))
    mixed = jnp.concatenate(mixed, axis=1)
    return (mixed, gate_ready[None], up_ready[None], down_ready[None])


def solution(mesh):
    placed = (
        P("fs", "tp"),
        P("fs"),
        P(None, "fs", "tp"),
        P(None, "fs", "tp"),
        P(None, "fs", "tp"),
        P("fs", None),
        P("fs", None),
    )

    def program(*arrays):
        step = jax.shard_map(
            shards,
            mesh=mesh,
            in_specs=placed,
            out_specs=(P("fs", "tp"), P("fs", None, "tp"), P("fs", None, "tp"), P("fs", None, "tp")),
            check_vma=False,
        )
        return step(*arrays)

    return program
```
